32 devices in a mesh: grp: 2 (over y), fs: 4 (over z), tp: 4 (over x, core).
Axes of the slice: x: 2, y: 2, z: 4, core: 2. Of those that a mesh axis runs over, the one named last changes fastest.
Arguments:
- tokens: bfloat16 [4096, 2048], P(('grp', 'fs'), 'tp'), parts along dimension 0, may hold values from -6 to 6
- first_gain: bfloat16 [2048], replicated, may hold values from 0.099609375 to 1.8984375
- u_proj: bfloat16 [2048, 1024], P('fs', 'tp'), may hold values from -0.125 to 0.125
- v_proj: bfloat16 [2048, 1024], P('fs', 'tp'), may hold values from -0.125 to 0.125
- group_gain: bfloat16 [8, 128], P('tp'), may hold values from 0.099609375 to 1.8984375
- spatial: bfloat16 [8, 128, 128], P('tp'), may hold values from -0.5 to 0.5
- spatial_bias: bfloat16 [8, 128], P('tp'), may hold values from 0.099609375 to 1.8984375
- mix_proj: bfloat16 [1024, 2048], P('fs', 'tp'), may hold values from -0.1875 to 0.1875
- second_gain: bfloat16 [2048], replicated, may hold values from 0.099609375 to 1.8984375
- up_proj: bfloat16 [2048, 8192], P('fs', 'tp'), may hold values from -0.125 to 0.125
- down_proj: bfloat16 [8192, 2048], P('tp', 'fs'), may hold values from -0.0625 to 0.0625
Outputs:
- layer_out: bfloat16 [4096, 2048], P(('grp', 'fs'), 'tp'), parts along dimension 0
The draws below stay inside these ranges and needn't reach their ends.
There are 2 independent parts, one for each index of `grp`. The reference program is written for one: setup_inputs(seed, part) draws one part's arguments, and reference() takes and returns one part's arrays. A program takes and returns all parts, laid end to end along the dimension named above; an argument that names none is the same for every part. Nothing has to cross between parts.
All inputs are finite; a program needn't handle non-finite values.
Results may differ from the reference program's by a relative error of at most 0.017.
Values may be sent and summed in bfloat16 or wider, within the bound.
A program may use at most 64 MiB of HBM per device.

```python
import jax
import jax.numpy as jnp
from jax import lax

D = 2048
GROUPS = 8
GROUP_DIM = 128
FF = 8192
BLOCK = 128
D_A = 1024
FF_DEV = 2048
TOKENS = 2048


def level_of(key, extent, cuts, least, high):
    level, own = 1.0, jax.random.fold_in(key, 6)
    for dim, shards_of in cuts:
        steps = jnp.exp(jax.random.uniform(jax.random.fold_in(own, dim), (shards_of,), jnp.float32, least / len(cuts), high / len(cuts)))
        level = level * jnp.repeat(steps, extent[dim] // shards_of).reshape([-1 if axis == dim else 1 for axis in range(len(extent))])
    return level


def bell_draw(own_key, extent, width, limit, split=(), kind=jnp.bfloat16):
    values = jax.random.normal(own_key, extent, jnp.float32) * width
    if len(split) > 0:
        values = level_of(own_key, extent, split, -0.22, 0.18) * values
    return jnp.clip(values, min=-limit, max=limit).astype(kind)


def setup_inputs(seed: int = 0, part: int = 0) -> dict:
    arg_keys = jax.random.split(jax.random.key(seed), 12)
    part_keys = jax.random.split(jax.random.fold_in(arg_keys[11], part), 12)
    return {
        "tokens": bell_draw(part_keys[0], (TOKENS, D), 1.0, 6.0, ((0, 4), (1, 4))),
        "first_gain": jnp.clip(1.0 + 0.18 * jax.random.normal(arg_keys[1], (D,), jnp.float32), 0.099609375, 1.8984375).astype(jnp.bfloat16),
        "u_proj": bell_draw(arg_keys[2], (D, D_A), D ** -0.5, 0.125, ((0, 4), (1, 4))),
        "v_proj": bell_draw(arg_keys[3], (D, D_A), D ** -0.5, 0.125, ((0, 4), (1, 4))),
        "group_gain": jnp.clip(1.0 + 0.18 * jax.random.normal(arg_keys[4], (GROUPS, GROUP_DIM), jnp.float32), 0.099609375, 1.8984375).astype(jnp.bfloat16),
        "spatial": bell_draw(arg_keys[5], (GROUPS, BLOCK, BLOCK), BLOCK ** -0.5, 0.5, ((0, 4),)),
        "spatial_bias": jnp.clip(1.0 + 0.18 * jax.random.normal(arg_keys[6], (GROUPS, BLOCK), jnp.float32), 0.099609375, 1.8984375).astype(jnp.bfloat16),
        "mix_proj": bell_draw(arg_keys[7], (D_A, D), D_A ** -0.5, 0.1875, ((0, 4), (1, 4))),
        "second_gain": jnp.clip(1.0 + 0.18 * jax.random.normal(arg_keys[8], (D,), jnp.float32), 0.099609375, 1.8984375).astype(jnp.bfloat16),
        "up_proj": bell_draw(arg_keys[9], (D, FF), D ** -0.5, 0.125, ((0, 4), (1, 4))),
        "down_proj": bell_draw(arg_keys[10], (FF, D), FF ** -0.5, 0.0625, ((0, 4), (1, 4))),
    }


EPS = 1e-06

def rms_scale(values, gain_vec):
    mean_sq = lax.optimization_barrier(jnp.mean(values * values, axis=-1, keepdims=True))
    return values * lax.rsqrt(mean_sq + EPS) * gain_vec.astype(jnp.float32)

def reference(tokens, first_gain, u_proj, v_proj, group_gain, spatial, spatial_bias, mix_proj, second_gain, up_proj, down_proj):
    row_count = tokens.shape[0]
    residual = tokens.astype(jnp.float32)
    normed_rows = rms_scale(residual, first_gain).astype(jnp.bfloat16)
    u_act = jax.nn.gelu(jnp.dot(normed_rows, u_proj, preferred_element_type=jnp.float32)).astype(jnp.bfloat16)
    v_act = jax.nn.gelu(jnp.dot(normed_rows, v_proj, preferred_element_type=jnp.float32))
    v_groups = v_act.reshape(row_count, GROUPS, GROUP_DIM)
    v_normed = rms_scale(v_groups, group_gain).astype(jnp.bfloat16)
    block_view = v_normed.reshape(row_count // BLOCK, BLOCK, GROUPS, GROUP_DIM)
    causal_mask = jnp.tril(jnp.ones((BLOCK, BLOCK), jnp.bool_))
    masked_weights = jnp.where(causal_mask[None], spatial, jnp.zeros_like(spatial))
    mixed_vals = jnp.einsum('gts,nsgd->ntgd', masked_weights.astype(jnp.float32), block_view.astype(jnp.float32))
    mixed_vals = mixed_vals + spatial_bias.astype(jnp.float32).T[None, :, :, None]
    gated_vals = (u_act.astype(jnp.float32) * mixed_vals.reshape(row_count, GROUPS * GROUP_DIM)).astype(jnp.bfloat16)
    mix_vals = jnp.dot(gated_vals, mix_proj, preferred_element_type=jnp.float32)
    mid_stream = (residual + mix_vals).astype(jnp.bfloat16)
    normed_two = rms_scale(mid_stream.astype(jnp.float32), second_gain).astype(jnp.bfloat16)
    pre_act = jnp.dot(normed_two, up_proj, preferred_element_type=jnp.float32)
    hidden_act = jnp.square(jax.nn.relu(pre_act)).astype(jnp.bfloat16)
    down_sum = jnp.zeros((row_count, D), jnp.float32)
    for block_idx in range(FF // FF_DEV):
        first_row = block_idx * FF_DEV
        partial_prod = jnp.dot(hidden_act[:, first_row:first_row + FF_DEV], down_proj[first_row:first_row + FF_DEV], preferred_element_type=jnp.float32)
        rounded_part = lax.optimization_barrier(partial_prod.astype(jnp.bfloat16))
        down_sum = down_sum + rounded_part.astype(jnp.float32)
    return (mid_stream.astype(jnp.float32) + down_sum).astype(jnp.bfloat16)
```

```python
import functools

import jax
import jax.numpy as jnp
from jax import lax
from jax.experimental import pallas as pl
from jax.experimental.pallas import tpu as pltpu
from jax.sharding import PartitionSpec as P

EPS = 1e-06


def rms_scale(values, gain_vec):
    mean_sq = jnp.mean(values * values, axis=-1, keepdims=True)
    return values * lax.rsqrt(mean_sq + EPS) * gain_vec.astype(jnp.float32)


def per_device(
    tokens,
    first_gain,
    u_proj,
    v_proj,
    group_gain,
    spatial,
    spatial_bias,
    mix_proj,
    second_gain,
    up_proj,
    down_proj,
):
    whole_rows = lax.all_gather(tokens, "tp", axis=1, tiled=True)
    row_count = whole_rows.shape[0]
    normed_rows = rms_scale(whole_rows.astype(jnp.float32), first_gain).astype(jnp.bfloat16)
    local_width = u_proj.shape[1]
    column_part = normed_rows
    u_pre = jnp.dot(
        column_part,
        lax.all_gather(u_proj, "fs", axis=0, tiled=True),
        preferred_element_type=jnp.float32,
    )
    v_pre = jnp.dot(
        column_part,
        lax.all_gather(v_proj, "fs", axis=0, tiled=True),
        preferred_element_type=jnp.float32,
    )
    u_act = jax.nn.gelu(u_pre).astype(jnp.bfloat16)
    local_groups = group_gain.shape[0]
    group_width = group_gain.shape[1]
    v_groups = jax.nn.gelu(v_pre).reshape(row_count, local_groups, group_width)
    v_normed = rms_scale(v_groups, group_gain).astype(jnp.bfloat16)
    block_len = spatial.shape[1]
    block_view = v_normed.reshape(row_count // block_len, block_len, local_groups, group_width)
    causal_mask = jnp.tril(jnp.ones((block_len, block_len), jnp.bool_))
    masked_weights = jnp.where(causal_mask[None], spatial, jnp.zeros_like(spatial))
    mixed_vals = jnp.einsum(
        "gts,nsgd->ntgd", masked_weights, block_view, preferred_element_type=jnp.float32
    )
    mixed_vals = mixed_vals + spatial_bias.astype(jnp.float32).T[None, :, :, None]
    gated_vals = (u_act.astype(jnp.float32) * mixed_vals.reshape(row_count, local_width)).astype(
        jnp.bfloat16
    )
    gated_whole = lax.all_gather(gated_vals, "tp", axis=1, tiled=True)
    column_part = gated_whole
    mix_vals = jnp.dot(
        column_part,
        lax.all_gather(mix_proj, "fs", axis=0, tiled=True),
        preferred_element_type=jnp.float32,
    )
    mid_stream = (tokens.astype(jnp.float32) + mix_vals).astype(jnp.bfloat16)
    mid_whole = lax.all_gather(mid_stream, "tp", axis=1, tiled=True)
    normed_two = rms_scale(mid_whole.astype(jnp.float32), second_gain).astype(jnp.bfloat16)
    column_part = normed_two
    pre_act = jnp.dot(
        column_part,
        lax.all_gather(up_proj, "fs", axis=0, tiled=True),
        preferred_element_type=jnp.float32,
    )
    hidden_act = jnp.square(jax.nn.relu(pre_act)).astype(jnp.bfloat16)
    down_terms = jnp.dot(
        hidden_act,
        lax.all_gather(down_proj, "fs", axis=1, tiled=True),
        preferred_element_type=jnp.float32,
    )
    down_sum = lax.psum_scatter(
        down_terms.astype(jnp.bfloat16), "tp", scatter_dimension=1, tiled=True
    ).astype(jnp.float32)
    return (mid_stream.astype(jnp.float32) + down_sum).astype(jnp.bfloat16)


def remote(src, dst, send, recv, where):
    return pltpu.make_async_remote_copy(
        src_ref=src,
        dst_ref=dst,
        send_sem=send,
        recv_sem=recv,
        device_id=where,
        device_id_type=pl.DeviceIdType.MESH,
    )


def fused_kernel(
    tok, gain1, u_w, v_w, ggain, spat, bias, mix_w, gain2, up_w, down_w,
    out,
    xg, uvg, mg, upg, dng, norm, gat, mid, hid, c_out, c_in, z_out, z_in, x_out, x_in,
    z_send, z_recv, y_send, y_recv, l_sem, a_send, a_recv, c_send, c_recv, r_send, r_recv,
    s_send, s_recv,
):
    y, z, t = lax.axis_index("grp"), lax.axis_index("fs"), lax.axis_index("tp")
    q, c, x = lax.rem(z, 2), lax.rem(t, 2), t // 2
    z_pair = z + 1 - 2 * q
    t_core, t_chip = t + 1 - 2 * c, lax.rem(t + 2, 4)
    to_y, to_z = (1 - y, z, t), (y, z_pair, t)
    to_c, to_x = (y, z, t_core), (y, z, t_chip)
    others = (lax.rem(z + 2, 4), 3 - z, z_pair)
    rows, width = tok.shape
    all_rows = 2 * rows
    step = 256
    f32, bf16 = jnp.float32, jnp.bfloat16

    barrier = pltpu.get_barrier_semaphore()
    for where in (to_y, to_c, to_x) + tuple((y, o, t) for o in others):
        pl.semaphore_signal(
            barrier, inc=1, device_id=where, device_id_type=pl.DeviceIdType.MESH
        )
    pl.semaphore_wait(barrier, 6)

    gw = ggain.shape[1]
    ur, mr, mc = u_w.shape[0], mix_w.shape[0], mix_w.shape[1] // 2
    pr, pc = up_w.shape[0], up_w.shape[1] // 2
    dr = down_w.shape[0] // 2

    def half(size, which):
        return pl.ds(pl.multiple_of(which * size, size), size)

    def take(w, par, which):
        if w == 0:
            return u_w.at[slice(None) if which is None else half(ur // 2, which), half(gw, par)]
        if w == 1:
            return v_w.at[slice(None) if which is None else half(ur // 2, which), half(gw, par)]
        if w == 2:
            return mix_w.at[slice(None) if which is None else half(mr // 2, which), half(mc, par)]
        if w == 3:
            return up_w.at[slice(None) if which is None else half(pr // 2, which), half(pc, par)]
        if which is None:
            return down_w.at[half(dr, par), :]
        return down_w.at[half(dr // 2, 2 * par + which), :]

    def put(w, source, which):
        if w < 2:
            cols = pl.ds(w * gw, gw)
            if which is None:
                return uvg.at[half(ur, source), cols]
            return uvg.at[half(ur // 2, 2 * source + which), cols]
        if w == 2:
            return mg.at[half(mr, source) if which is None else half(mr // 2, 2 * source + which), :]
        if w == 3:
            return upg.at[half(pr, source) if which is None else half(pr // 2, 2 * source + which), :]
        if which is None:
            return dng.at[source]
        return dng.at[source, half(dr // 2, which), :]

    def z_copy(w, dest):
        return remote(
            take(w, lax.rem(dest, 2), y), put(w, z, y), z_send.at[w, dest], z_recv.at[w, z],
            (y, dest, t),
        )

    def z_arrived(w, source):
        return remote(
            put(w, source, y), put(w, source, y), z_send.at[w, source], z_recv.at[w, source],
            (y, source, t),
        )

    def y_copy(w, source):
        return remote(
            put(w, source, y), put(w, source, y), y_send.at[w, source], y_recv.at[w, source], to_y
        )

    def y_arrived(w, source):
        return remote(
            put(w, source, 1 - y), put(w, source, 1 - y), y_send.at[w, source],
            y_recv.at[w, source], to_y,
        )

    def forward(w, source):
        z_arrived(w, source).wait_recv()
        y_copy(w, source).start()

    def own_copy(w):
        return pltpu.make_async_copy(take(w, q, None), put(w, z, None), l_sem.at[w])

    def gather_copy(buf, a, n):
        p, s, where = (
            (q, t, to_z), (q, t, to_x), (q, t, to_c), (1 - q, t, to_x), (1 - q, t, to_c),
            (q, t_chip, to_c), (1 - q, t_chip, to_c),
        )[n]
        return remote(
            buf.at[p, s], buf.at[p, s], a_send.at[a, n], a_recv.at[a, n], where
        )

    def gather_arrived(buf, a, n):
        p, s, where = (
            (1 - q, t, to_z), (q, t_chip, to_x), (q, t_core, to_c), (1 - q, t_chip, to_x),
            (1 - q, t_core, to_c), (q, 3 - t, to_c), (1 - q, 3 - t, to_c),
        )[n]
        return remote(
            buf.at[p, s], buf.at[p, s], a_send.at[a, n], a_recv.at[a, n], where
        )

    def gather_start(buf, a):
        for n in (0, 1, 2):
            gather_copy(buf, a, n).start()

    def gather_finish(buf, a):
        gather_arrived(buf, a, 0).wait_recv()
        gather_copy(buf, a, 3).start()
        gather_copy(buf, a, 4).start()
        gather_arrived(buf, a, 1).wait_recv()
        gather_copy(buf, a, 5).start()
        gather_arrived(buf, a, 3).wait_recv()
        gather_copy(buf, a, 6).start()
        for n in (2, 4, 5, 6):
            gather_arrived(buf, a, n).wait_recv()

    own_tok = pltpu.make_async_copy(tok, xg.at[q, t], l_sem.at[5])
    own_tok.start()
    own_tok.wait()
    gather_start(xg, 0)
    for w in range(5):
        own_copy(w).start()
    for w in range(3):
        for o in others:
            z_copy(w, o).start()
    for o in others[:2]:
        z_copy(3, o).start()

    gather_finish(xg, 0)
    for w in range(3):
        for o in others:
            forward(w, o)

    def scaled(pieces, gain):
        total = pieces[0].shape[0]
        sums = jnp.zeros((total, 1), f32)
        for piece in pieces:
            sums += jnp.sum(piece * piece, axis=-1, keepdims=True)
        count = sum(piece.shape[1] for piece in pieces)
        scale = lax.rsqrt(sums / count + EPS)
        at = 0
        res = []
        for piece in pieces:
            wide = piece.shape[1]
            res.append((piece * scale * gain[:, at : at + wide]).astype(bf16))
            at += wide
        return jnp.concatenate(res, axis=1)

    small = 64
    per_part = rows // small
    gain_one = gain1[...].astype(f32)
    gain_two = gain2[...].astype(f32)

    def norm_one(i, carry):
        p, r = i // per_part, pl.multiple_of(lax.rem(i, per_part) * small, small)
        pieces = [xg[p, s, pl.ds(r, small), :].astype(f32) for s in range(4)]
        norm[pl.ds(pl.multiple_of(i * small, small), small), :] = scaled(pieces, gain_one)
        return carry

    lax.fori_loop(0, all_rows // small, norm_one, 0)

    for w in range(2):
        own_copy(w).wait()
        for o in others:
            y_arrived(w, o).wait_recv()

    blk = spat.shape[1]
    lower = lax.broadcasted_iota(jnp.int32, (blk, blk), 0) >= lax.broadcasted_iota(
        jnp.int32, (blk, blk), 1
    )
    mixer = jnp.where(lower, spat[q].astype(f32), 0.0).astype(bf16)
    shift = jnp.where(q == 0, bias[:, 0:1], bias[:, 1:2])
    gain_g = jnp.where(q == 0, ggain[0:1, :], ggain[1:2, :])

    def mix_rows(i, carry):
        here = pl.ds(pl.multiple_of(i * step, step), step)
        both = jnp.dot(norm[here, :], uvg[...], preferred_element_type=f32)
        both = jax.nn.gelu(both)
        u_act = both[:, :gw].astype(bf16).astype(f32)
        v_act = both[:, gw:]
        v_n = (
            v_act
            * lax.rsqrt(jnp.mean(v_act * v_act, axis=-1, keepdims=True) + EPS)
            * gain_g
        ).astype(bf16)
        for b in range(step // blk):
            part = slice(b * blk, (b + 1) * blk)
            mixed = jnp.dot(mixer, v_n[part], preferred_element_type=f32) + shift
            gat[q, t, pl.ds(pl.multiple_of(i * step + b * blk, blk), blk), :] = (
                u_act[part] * mixed
            ).astype(bf16)
        return carry

    lax.fori_loop(0, all_rows // step, mix_rows, 0)
    gather_start(gat, 1)
    z_copy(3, others[2]).start()
    for o in others[:2]:
        z_copy(4, o).start()
    gather_finish(gat, 1)
    own_copy(2).wait()
    for o in others:
        y_arrived(2, o).wait_recv()

    def middle_rows(i, carry):
        here = pl.ds(pl.multiple_of(i * step, step), step)
        p = i // (rows // step)
        within = pl.ds(pl.multiple_of(lax.rem(i, rows // step) * step, step), step)
        left = jnp.concatenate([gat[k % 2, k // 2, here, :] for k in range(8)], axis=1)
        value = jnp.dot(left, mg[...], preferred_element_type=f32)
        value += xg[p, t, within, half(mc, q)].astype(f32)
        mid[q, t, here, :] = value.astype(bf16)
        return carry

    lax.fori_loop(0, all_rows // step, middle_rows, 0)
    gather_start(mid, 2)
    z_copy(4, others[2]).start()
    for o in others[:2]:
        forward(3, o)
    gather_finish(mid, 2)
    forward(3, others[2])

    def norm_two(i, carry):
        here = pl.ds(pl.multiple_of(i * small, small), small)
        pieces = [mid[k % 2, k // 2, here, :].astype(f32) for k in range(8)]
        norm[here, :] = scaled(pieces, gain_two)
        return carry

    lax.fori_loop(0, all_rows // small, norm_two, 0)
    own_copy(3).wait()
    for o in others:
        y_arrived(3, o).wait_recv()

    def up_rows(i, carry):
        here = pl.ds(pl.multiple_of(i * step, step), step)
        pre = jnp.dot(norm[here, :], upg[...], preferred_element_type=f32)
        hid[here, :] = jnp.square(jax.nn.relu(pre)).astype(bf16)
        return carry

    lax.fori_loop(0, all_rows // step, up_rows, 0)

    near, far = z // 2, 1 - z // 2
    order = (2 * near + 1 - c, 2 * near + c, 2 * far + 1 - c, 2 * far + c)

    def fetch(quarter):
        @pl.when(quarter != z)
        def _():
            forward(4, quarter)

    def ready(quarter):
        @pl.when(quarter == z)
        def _():
            own_copy(4).wait()

        @pl.when(quarter != z)
        def _():
            y_arrived(4, quarter).wait_recv()

    def down_part(quarter, start):
        return jnp.dot(
            hid[pl.ds(start, step), :], dng[quarter], preferred_element_type=f32
        )

    def core_copy(n):
        return remote(c_out.at[n], c_in.at[n], c_send.at[n], c_recv.at[n], to_c)

    def pair_copy(n):
        return remote(z_out.at[n], z_in.at[n], r_send.at[n], r_recv.at[n], to_z)

    def chip_copy():
        return remote(x_out, x_in, s_send.at[0], s_recv.at[0], to_x)

    def give(n):
        quarter = order[2 * n]
        ready(quarter)

        def loop(i, carry):
            start = pl.multiple_of(i * step, step)
            c_out[n, pl.ds(start, step), :] = down_part(quarter, start).astype(bf16)
            return carry

        lax.fori_loop(0, all_rows // step, loop, 0)
        core_copy(n).start()

    def keep(n):
        quarter = order[2 * n + 1]
        ready(quarter)
        core_copy(n).wait_recv()

        def loop_other(i, carry):
            off = pl.multiple_of(i * step, step)
            start = pl.multiple_of((1 - q) * rows + i * step, step)
            value = down_part(quarter, start) + c_in[n, pl.ds(start, step), :].astype(f32)
            z_out[n, pl.ds(off, step), :] = value.astype(bf16)
            return carry

        lax.fori_loop(0, rows // step, loop_other, 0)
        pair_copy(n).start()

        def loop_own(i, carry):
            off = pl.multiple_of(i * step, step)
            start = pl.multiple_of(q * rows + i * step, step)
            value = down_part(quarter, start) + c_in[n, pl.ds(start, step), :].astype(f32)
            c_in[n, pl.ds(start, step), :] = value.astype(bf16)
            return carry

        lax.fori_loop(0, rows // step, loop_own, 0)

    fetch(order[0])
    fetch(order[1])
    give(0)
    fetch(order[2])
    keep(0)
    fetch(order[3])
    give(1)
    keep(1)

    mine = pl.ds(pl.multiple_of(q * rows, rows), rows)

    def total(n, i):
        off = pl.multiple_of(i * step, step)
        start = pl.multiple_of(q * rows + i * step, step)
        return c_in[n, pl.ds(start, step), :].astype(f32) + z_in[n, pl.ds(off, step), :].astype(f32)

    far_slot = jnp.where(near == x, 1, 0)
    own_slot = 1 - far_slot

    def send_far(i, carry):
        x_out[pl.ds(pl.multiple_of(i * step, step), step), :] = total(far_slot, i).astype(bf16)
        return carry

    def finish(i, carry):
        off = pl.multiple_of(i * step, step)
        here = pl.ds(pl.multiple_of(q * rows + i * step, step), step)
        value = total(own_slot, i) + x_in[pl.ds(off, step), :].astype(f32)
        stream = jnp.concatenate([mid[0, t, here, :], mid[1, t, here, :]], axis=1)
        out[pl.ds(off, step), :] = (value + stream.astype(f32)).astype(bf16)
        return carry

    pair_copy(0).wait_recv()

    @pl.when(far_slot == 0)
    def _():
        lax.fori_loop(0, rows // step, send_far, 0)
        chip_copy().start()

    pair_copy(1).wait_recv()

    @pl.when(far_slot == 1)
    def _():
        lax.fori_loop(0, rows // step, send_far, 0)
        chip_copy().start()

    chip_copy().wait_recv()
    lax.fori_loop(0, rows // step, finish, 0)

    for w in range(5):
        for o in others:
            z_copy(w, o).wait_send()
            y_copy(w, o).wait_send()
    for a, buf in enumerate((xg, gat, mid)):
        for n in range(7):
            gather_copy(buf, a, n).wait_send()
    for n in range(2):
        core_copy(n).wait_send()
        pair_copy(n).wait_send()
    chip_copy().wait_send()


def fused(tokens, first_gain, u_proj, v_proj, group_gain, spatial, spatial_bias, mix_proj,
          second_gain, up_proj, down_proj):
    rows, width = tokens.shape
    both, wide, gw = 2 * rows, second_gain.shape[0], group_gain.shape[1]
    vmem, bf16, dma = pltpu.VMEM, jnp.bfloat16, pltpu.SemaphoreType.DMA
    spec = pl.BlockSpec(memory_space=pltpu.VMEM)
    ff = up_proj.shape[1] // 2
    return pl.pallas_call(
        fused_kernel,
        out_shape=jax.ShapeDtypeStruct(tokens.shape, tokens.dtype),
        in_specs=[spec] * 11,
        out_specs=spec,
        scratch_shapes=[
            vmem((2, 4, rows, width), bf16),
            vmem((wide, 2 * gw), bf16),
            vmem((4 * mix_proj.shape[0], width // 2), bf16),
            vmem((wide, ff), bf16),
            vmem((4, ff, down_proj.shape[1]), bf16),
            vmem((both, wide), bf16),
            vmem((2, 4, both, gw), bf16),
            vmem((2, 4, both, width // 2), bf16),
            vmem((both, ff), bf16),
            vmem((2, both, width), bf16),
            vmem((2, both, width), bf16),
            vmem((2, rows, width), bf16),
            vmem((2, rows, width), bf16),
            vmem((rows, width), bf16),
            vmem((rows, width), bf16),
            dma((5, 4)), dma((5, 4)), dma((5, 4)), dma((5, 4)), dma((6,)),
            dma((3, 7)), dma((3, 7)), dma((2,)), dma((2,)), dma((2,)), dma((2,)),
            dma((1,)), dma((1,)),
        ],
        compiler_params=pltpu.CompilerParams(
            collective_id=0, has_side_effects=True, vmem_limit_bytes=64 * 1024 * 1000
        ),
    )(
        tokens, first_gain[None], u_proj, v_proj, group_gain.astype(jnp.float32), spatial,
        spatial_bias.astype(jnp.float32).T, mix_proj, second_gain[None], up_proj, down_proj,
    )


def layer_part(axes, *args):
    tokens, group_gain, spatial = args[0], args[4], args[5]
    fits = (
        axes["grp"] == 2
        and axes["fs"] == 4
        and axes["tp"] == 4
        and group_gain.shape[0] == 2
        and group_gain.shape[1] % 128 == 0
        and tokens.shape[0] % 256 == 0
        and tokens.shape[1] % 256 == 0
        and tokens.shape[1] == args[10].shape[1]
        and 256 % spatial.shape[1] == 0
    )
    return fused(*args) if fits else per_device(*args)


def solution(mesh):
    return jax.shard_map(
        functools.partial(layer_part, dict(mesh.shape)),
        mesh=mesh,
        in_specs=(
            P(("grp", "fs"), "tp"),
            P(),
            P("fs", "tp"),
            P("fs", "tp"),
            P("tp", None),
            P("tp", None, None),
            P("tp", None),
            P("fs", "tp"),
            P(),
            P("fs", "tp"),
            P("tp", "fs"),
        ),
        out_specs=P(("grp", "fs"), "tp"),
        check_vma=False,
    )
```

```python
import functools

import jax
import jax.numpy as jnp
from jax import lax
from jax.experimental import pallas as pl
from jax.experimental.pallas import tpu as pltpu
from jax.sharding import PartitionSpec as P

EPS = 1e-06


def rms_scale(values, gain_vec):
    mean_sq = jnp.mean(values * values, axis=-1, keepdims=True)
    return values * lax.rsqrt(mean_sq + EPS) * gain_vec.astype(jnp.float32)


def per_device(
    tokens,
    first_gain,
    u_proj,
    v_proj,
    group_gain,
    spatial,
    spatial_bias,
    mix_proj,
    second_gain,
    up_proj,
    down_proj,
):
    whole_rows = lax.all_gather(tokens, "tp", axis=1, tiled=True)
    row_count = whole_rows.shape[0]
    normed_rows = rms_scale(whole_rows.astype(jnp.float32), first_gain).astype(jnp.bfloat16)
    local_width = u_proj.shape[1]
    column_part = normed_rows
    u_pre = jnp.dot(
        column_part,
        lax.all_gather(u_proj, "fs", axis=0, tiled=True),
        preferred_element_type=jnp.float32,
    )
    v_pre = jnp.dot(
        column_part,
        lax.all_gather(v_proj, "fs", axis=0, tiled=True),
        preferred_element_type=jnp.float32,
    )
    u_act = jax.nn.gelu(u_pre).astype(jnp.bfloat16)
    local_groups = group_gain.shape[0]
    group_width = group_gain.shape[1]
    v_groups = jax.nn.gelu(v_pre).reshape(row_count, local_groups, group_width)
    v_normed = rms_scale(v_groups, group_gain).astype(jnp.bfloat16)
    block_len = spatial.shape[1]
    block_view = v_normed.reshape(row_count // block_len, block_len, local_groups, group_width)
    causal_mask = jnp.tril(jnp.ones((block_len, block_len), jnp.bool_))
    masked_weights = jnp.where(causal_mask[None], spatial, jnp.zeros_like(spatial))
    mixed_vals = jnp.einsum(
        "gts,nsgd->ntgd", masked_weights, block_view, preferred_element_type=jnp.float32
    )
    mixed_vals = mixed_vals + spatial_bias.astype(jnp.float32).T[None, :, :, None]
    gated_vals = (u_act.astype(jnp.float32) * mixed_vals.reshape(row_count, local_width)).astype(
        jnp.bfloat16
    )
    gated_whole = lax.all_gather(gated_vals, "tp", axis=1, tiled=True)
    column_part = gated_whole
    mix_vals = jnp.dot(
        column_part,
        lax.all_gather(mix_proj, "fs", axis=0, tiled=True),
        preferred_element_type=jnp.float32,
    )
    mid_stream = (tokens.astype(jnp.float32) + mix_vals).astype(jnp.bfloat16)
    mid_whole = lax.all_gather(mid_stream, "tp", axis=1, tiled=True)
    normed_two = rms_scale(mid_whole.astype(jnp.float32), second_gain).astype(jnp.bfloat16)
    column_part = normed_two
    pre_act = jnp.dot(
        column_part,
        lax.all_gather(up_proj, "fs", axis=0, tiled=True),
        preferred_element_type=jnp.float32,
    )
    hidden_act = jnp.square(jax.nn.relu(pre_act)).astype(jnp.bfloat16)
    down_terms = jnp.dot(
        hidden_act,
        lax.all_gather(down_proj, "fs", axis=1, tiled=True),
        preferred_element_type=jnp.float32,
    )
    down_sum = lax.psum_scatter(
        down_terms.astype(jnp.bfloat16), "tp", scatter_dimension=1, tiled=True
    ).astype(jnp.float32)
    return (mid_stream.astype(jnp.float32) + down_sum).astype(jnp.bfloat16)


def remote(src, dst, send, recv, where):
    return pltpu.make_async_remote_copy(
        src_ref=src,
        dst_ref=dst,
        send_sem=send,
        recv_sem=recv,
        device_id=where,
        device_id_type=pl.DeviceIdType.MESH,
    )


def fused_kernel(
    row_step,
    tok, gain1, u_w, v_w, ggain, spat, bias, mix_w, gain2, up_w, down_w,
    out,
    xg, uvg, mg, upg, dng, norm, gat, mid, hid, c_out, c_in, z_out, z_in, x_out, x_in,
    z_send, z_recv, y_send, y_recv, l_sem, a_send, a_recv, c_send, c_recv, r_send, r_recv,
    s_send, s_recv,
):
    y, z, t = lax.axis_index("grp"), lax.axis_index("fs"), lax.axis_index("tp")
    q, c, x = lax.rem(z, 2), lax.rem(t, 2), t // 2
    z_pair = z + 1 - 2 * q
    t_core, t_chip = t + 1 - 2 * c, lax.rem(t + 2, 4)
    to_y, to_z = (1 - y, z, t), (y, z_pair, t)
    to_c, to_x = (y, z, t_core), (y, z, t_chip)
    others = (lax.rem(z + 2, 4), 3 - z, z_pair)
    rows, width = tok.shape
    step = row_step
    f32, bf16 = jnp.float32, jnp.bfloat16

    barrier = pltpu.get_barrier_semaphore()
    for where in (to_y, to_c, to_x) + tuple((y, o, t) for o in others):
        pl.semaphore_signal(
            barrier, inc=1, device_id=where, device_id_type=pl.DeviceIdType.MESH
        )
    pl.semaphore_wait(barrier, 6)

    gw = ggain.shape[1]
    ur, mr, mc = u_w.shape[0], mix_w.shape[0], mix_w.shape[1] // 2
    pr, pc = up_w.shape[0], up_w.shape[1] // 2
    dr = down_w.shape[0] // 2

    def half(size, which):
        return pl.ds(pl.multiple_of(which * size, size), size)

    def take(w, par, which):
        if w == 0:
            return u_w.at[slice(None) if which is None else half(ur // 2, which), half(gw, par)]
        if w == 1:
            return v_w.at[slice(None) if which is None else half(ur // 2, which), half(gw, par)]
        if w == 2:
            return mix_w.at[slice(None) if which is None else half(mr // 2, which), half(mc, par)]
        if w == 3:
            return up_w.at[slice(None) if which is None else half(pr // 2, which), half(pc, par)]
        if which is None:
            return down_w.at[half(dr, par), :]
        return down_w.at[half(dr // 2, 2 * par + which), :]

    def put(w, source, which):
        if w < 2:
            cols = pl.ds(w * gw, gw)
            if which is None:
                return uvg.at[half(ur, source), cols]
            return uvg.at[half(ur // 2, 2 * source + which), cols]
        if w == 2:
            return mg.at[half(mr, source) if which is None else half(mr // 2, 2 * source + which), :]
        if w == 3:
            return upg.at[half(pr, source) if which is None else half(pr // 2, 2 * source + which), :]
        if which is None:
            return dng.at[source]
        return dng.at[source, half(dr // 2, which), :]

    def z_copy(w, dest):
        return remote(
            take(w, lax.rem(dest, 2), y), put(w, z, y), z_send.at[w, dest], z_recv.at[w, z],
            (y, dest, t),
        )

    def z_arrived(w, source):
        return remote(
            put(w, source, y), put(w, source, y), z_send.at[w, source], z_recv.at[w, source],
            (y, source, t),
        )

    def y_copy(w, source):
        return remote(
            put(w, source, y), put(w, source, y), y_send.at[w, source], y_recv.at[w, source], to_y
        )

    def y_arrived(w, source):
        return remote(
            put(w, source, 1 - y), put(w, source, 1 - y), y_send.at[w, source],
            y_recv.at[w, source], to_y,
        )

    def forward(w, source):
        z_arrived(w, source).wait_recv()
        y_copy(w, source).start()

    def own_copy(w):
        return pltpu.make_async_copy(take(w, q, None), put(w, z, None), l_sem.at[w])

    def gather_copy(a, h, n):
        p, s, where = (
            (q, t, to_z), (q, t, to_x), (q, t, to_c), (1 - q, t, to_x), (1 - q, t, to_c),
            (q, t_chip, to_c), (1 - q, t_chip, to_c),
        )[n]
        ref = piece(a, h, p, s)
        return remote(ref, ref, a_send.at[a, h, n], a_recv.at[a, h, n], where)

    def gather_arrived(a, h, n):
        p, s, where = (
            (1 - q, t, to_z), (q, t_chip, to_x), (q, t_core, to_c), (1 - q, t_chip, to_x),
            (1 - q, t_core, to_c), (q, 3 - t, to_c), (1 - q, 3 - t, to_c),
        )[n]
        ref = piece(a, h, p, s)
        return remote(ref, ref, a_send.at[a, h, n], a_recv.at[a, h, n], where)

    def piece(a, h, p, s):
        if a == 0:
            return xg.at[p, s, pl.ds(h * step, step), :]
        return (gat, mid)[a - 1].at[p, s, h]

    def gather_start(a, h):
        for n in (0, 1, 2):
            gather_copy(a, h, n).start()

    def gather_pair(a, h):
        gather_arrived(a, h, 0).wait_recv()
        gather_copy(a, h, 3).start()
        gather_copy(a, h, 4).start()

    def gather_rest(a, h):
        gather_arrived(a, h, 1).wait_recv()
        gather_copy(a, h, 5).start()
        gather_arrived(a, h, 3).wait_recv()
        gather_copy(a, h, 6).start()
        for n in (2, 4, 5, 6):
            gather_arrived(a, h, n).wait_recv()

    chunks = rows // step
    inner = (z + 1) // 2 == 1
    across, facing, pair = others

    own_tok = pltpu.make_async_copy(tok, xg.at[q, t], l_sem.at[5])
    own_tok.start()
    for w in range(2):
        for o in others:
            z_copy(w, o).start()
    own_tok.wait()
    for h in range(chunks):
        gather_start(0, h)
    for w in range(5):
        own_copy(w).start()

    @pl.when(inner)
    def _():
        z_copy(2, facing).start()
        z_copy(3, facing).start()

    for h in range(chunks):
        gather_pair(0, h)

    @pl.when(jnp.logical_not(inner))
    def _():
        z_copy(2, facing).start()

    for o in (across, pair):
        z_copy(2, o).start()
    z_copy(3, across).start()
    for w in range(2):
        for o in others:
            forward(w, o)

    def scaled(pieces, gain):
        total = pieces[0].shape[0]
        sums = jnp.zeros((total, 1), f32)
        for piece in pieces:
            sums += jnp.sum(piece * piece, axis=-1, keepdims=True)
        count = sum(piece.shape[1] for piece in pieces)
        scale = lax.rsqrt(sums / count + EPS)
        at = 0
        res = []
        for piece in pieces:
            wide = piece.shape[1]
            res.append((piece * scale * gain[:, at : at + wide]).astype(bf16))
            at += wide
        return jnp.concatenate(res, axis=1)

    small = 64
    per_part = step // small
    gain_one = gain1[...].astype(f32).reshape(1, -1)
    gain_two = gain2[...].astype(f32).reshape(1, -1)

    def norm_one(h):
        def loop(i, carry):
            p, r = i // per_part, pl.multiple_of(lax.rem(i, per_part) * small, small)
            pieces = [xg[p, s, pl.ds(h * step + r, small), :].astype(f32) for s in range(4)]
            at = pl.multiple_of(h * 2 * step + i * small, small)
            norm[pl.ds(at, small), :] = scaled(pieces, gain_one)
            return carry

        lax.fori_loop(0, 2 * per_part, loop, 0)

    blk = spat.shape[1]
    lower = lax.broadcasted_iota(jnp.int32, (blk, blk), 0) >= lax.broadcasted_iota(
        jnp.int32, (blk, blk), 1
    )
    mixer = jnp.where(lower, spat[q].astype(f32), 0.0).astype(bf16)
    eye = lax.broadcasted_iota(jnp.int32, (blk, blk), 0) == lax.broadcasted_iota(
        jnp.int32, (blk, blk), 1
    )
    bias_row = jnp.where(q == 0, bias[0:1, :].astype(f32), bias[1:2, :].astype(f32))
    shift = jnp.sum(jnp.where(eye, bias_row, 0.0), axis=1, keepdims=True)
    gain_g = jnp.where(q == 0, ggain[0:1, :].astype(f32), ggain[1:2, :].astype(f32))

    def mix_rows(h):
        def loop(i, carry):
            here = pl.ds(pl.multiple_of((2 * h + i) * step, step), step)
            both = jnp.dot(norm[here, :], uvg[...], preferred_element_type=f32)
            both = jax.nn.gelu(both)
            u_act = both[:, :gw].astype(bf16).astype(f32)
            v_act = both[:, gw:]
            v_n = (
                v_act
                * lax.rsqrt(jnp.mean(v_act * v_act, axis=-1, keepdims=True) + EPS)
                * gain_g
            ).astype(bf16)
            for b in range(step // blk):
                part = slice(b * blk, (b + 1) * blk)
                mixed = jnp.dot(mixer, v_n[part], preferred_element_type=f32) + shift
                at = pl.multiple_of(i * step + b * blk, blk)
                gat[q, t, h, pl.ds(at, blk), :] = (u_act[part] * mixed).astype(bf16)
            return carry

        lax.fori_loop(0, 2, loop, 0)

    def middle_rows(h):
        def loop(p, carry):
            here = pl.ds(pl.multiple_of(p * step, step), step)
            left = jnp.concatenate([gat[k % 2, k // 2, h, here, :] for k in range(8)], axis=1)
            value = jnp.dot(left, mg[...], preferred_element_type=f32)
            value += xg[p, t, pl.ds(h * step, step), half(mc, q)].astype(f32)
            mid[q, t, h, here, :] = value.astype(bf16)
            return carry

        lax.fori_loop(0, 2, loop, 0)

    def norm_two(h):
        def loop(i, carry):
            here = pl.ds(pl.multiple_of(i * small, small), small)
            pieces = [mid[k % 2, k // 2, h, here, :].astype(f32) for k in range(8)]
            at = pl.multiple_of(h * 2 * step + i * small, small)
            norm[pl.ds(at, small), :] = scaled(pieces, gain_two)
            return carry

        lax.fori_loop(0, 2 * per_part, loop, 0)

    def up_rows(h):
        def loop(i, carry):
            here = pl.ds(pl.multiple_of((2 * h + i) * step, step), step)
            pre = jnp.dot(norm[here, :], upg[...], preferred_element_type=f32)
            hid[here, :] = jnp.square(jax.nn.relu(pre)).astype(bf16)
            return carry

        lax.fori_loop(0, 2, loop, 0)

    for h in range(chunks):
        gather_rest(0, h)
        norm_one(h)
        if h == 0:
            for w in range(2):
                own_copy(w).wait()
                for o in others:
                    y_arrived(w, o).wait_recv()
        mix_rows(h)
        gather_start(1, h)

    @pl.when(inner)
    def _():
        z_copy(4, facing).start()

    @pl.when(jnp.logical_not(inner))
    def _():
        z_copy(3, facing).start()

    for o in others:
        forward(2, o)

    @pl.when(inner)
    def _():
        forward(3, facing)

    own_copy(2).wait()
    for h in range(chunks):
        gather_pair(1, h)
    for h in range(chunks):
        gather_rest(1, h)
        if h == 0:
            for o in others:
                y_arrived(2, o).wait_recv()
        middle_rows(h)
        gather_start(2, h)
    z_copy(3, pair).start()
    z_copy(4, across).start()
    z_copy(4, pair).start()

    @pl.when(jnp.logical_not(inner))
    def _():
        z_copy(4, facing).start()

    forward(3, across)
    for h in range(chunks):
        gather_pair(2, h)

    @pl.when(jnp.logical_not(inner))
    def _():
        forward(3, facing)

    for h in range(chunks):
        gather_rest(2, h)
        norm_two(h)

    @pl.when(inner)
    def _():
        forward(4, facing)

    forward(3, pair)
    own_copy(3).wait()
    for o in others:
        y_arrived(3, o).wait_recv()
    for h in range(chunks):
        up_rows(h)

    near, far = z // 2, 1 - z // 2
    order = (2 * near + 1 - c, 2 * near + c, 2 * far + 1 - c, 2 * far + c)

    def ready(quarter):
        @pl.when(quarter == z)
        def _():
            own_copy(4).wait()

        @pl.when(quarter != z)
        def _():
            y_arrived(4, quarter).wait_recv()

    def down_part(quarter, h, p):
        start = pl.multiple_of((2 * h + p) * step, step)
        return jnp.dot(
            hid[pl.ds(start, step), :], dng[quarter], preferred_element_type=f32
        )

    def core_copy(n, h, p):
        return remote(
            c_out.at[n, h, p], c_in.at[n, h, p], c_send.at[n, h, p], c_recv.at[n, h, p], to_c
        )

    def pair_copy(n, h):
        return remote(z_out.at[n, h], z_in.at[n, h], r_send.at[n, h], r_recv.at[n, h], to_z)

    def chip_copy(h):
        return remote(x_out.at[h], x_in.at[h], s_send.at[h], s_recv.at[h], to_x)

    def give(n):
        quarter = order[2 * n]
        ready(quarter)
        for i in range(2 * chunks):
            h, p = i % chunks, (1 - q if i < chunks else q)
            c_out[n, h, p] = down_part(quarter, h, p).astype(bf16)
            core_copy(n, h, p).start()

    def keep(n):
        quarter = order[2 * n + 1]
        ready(quarter)
        for i in range(2 * chunks):
            h, p = i % chunks, (1 - q if i < chunks else q)
            core_copy(n, h, p).wait_recv()
            value = down_part(quarter, h, p) + c_in[n, h, p].astype(f32)
            if i < chunks:
                z_out[n, h] = value.astype(bf16)
                pair_copy(n, h).start()
            else:
                c_in[n, h, p] = value.astype(bf16)

    forward(4, across)
    forward(4, pair)
    give(0)

    @pl.when(jnp.logical_not(inner))
    def _():
        forward(4, facing)

    keep(0)
    give(1)
    keep(1)

    far_slot = jnp.where(near == x, 1, 0)
    own_slot = 1 - far_slot

    def send_far(n):
        for h in range(chunks):
            pair_copy(n, h).wait_recv()
            value = c_in[n, h, q].astype(f32) + z_in[n, h].astype(f32)
            x_out[h] = value.astype(bf16)
            chip_copy(h).start()

    @pl.when(far_slot == 0)
    def _():
        send_far(0)
        for h in range(chunks):
            pair_copy(1, h).wait_recv()

    @pl.when(far_slot == 1)
    def _():
        for h in range(chunks):
            pair_copy(0, h).wait_recv()
        send_far(1)

    for h in range(chunks):
        chip_copy(h).wait_recv()
        value = c_in[own_slot, h, q].astype(f32) + z_in[own_slot, h].astype(f32)
        value += x_in[h].astype(f32)
        here = pl.ds(pl.multiple_of(q * step, step), step)
        stream = jnp.concatenate([mid[0, t, h, here, :], mid[1, t, h, here, :]], axis=1)
        out[pl.ds(h * step, step), :] = (value + stream.astype(f32)).astype(bf16)

    for w in range(5):
        for o in others:
            z_copy(w, o).wait_send()
            y_copy(w, o).wait_send()
    for h in range(chunks):
        for a in range(3):
            for n in range(7):
                gather_copy(a, h, n).wait_send()
        for n in range(2):
            for p in range(2):
                core_copy(n, h, p).wait_send()
            pair_copy(n, h).wait_send()
        chip_copy(h).wait_send()


def fused(tokens, first_gain, u_proj, v_proj, group_gain, spatial, spatial_bias, mix_proj,
          second_gain, up_proj, down_proj):
    rows, width = tokens.shape
    both, wide, gw = 2 * rows, second_gain.shape[0], group_gain.shape[1]
    vmem, bf16, dma = pltpu.VMEM, jnp.bfloat16, pltpu.SemaphoreType.DMA
    spec = pl.BlockSpec(memory_space=pltpu.VMEM)
    ff = up_proj.shape[1] // 2
    step = 256
    chunks = rows // step
    return pl.pallas_call(
        functools.partial(fused_kernel, step),
        out_shape=jax.ShapeDtypeStruct(tokens.shape, tokens.dtype),
        in_specs=[spec] * 11,
        out_specs=spec,
        scratch_shapes=[
            vmem((2, 4, rows, width), bf16),
            vmem((wide, 2 * gw), bf16),
            vmem((4 * mix_proj.shape[0], width // 2), bf16),
            vmem((wide, ff), bf16),
            vmem((4, ff, down_proj.shape[1]), bf16),
            vmem((both, wide), bf16),
            vmem((2, 4, chunks, 2 * step, gw), bf16),
            vmem((2, 4, chunks, 2 * step, width // 2), bf16),
            vmem((both, ff), bf16),
            vmem((2, chunks, 2, step, width), bf16),
            vmem((2, chunks, 2, step, width), bf16),
            vmem((2, chunks, step, width), bf16),
            vmem((2, chunks, step, width), bf16),
            vmem((chunks, step, width), bf16),
            vmem((chunks, step, width), bf16),
            dma((5, 4)), dma((5, 4)), dma((5, 4)), dma((5, 4)), dma((6,)),
            dma((3, chunks, 7)), dma((3, chunks, 7)),
            dma((2, chunks, 2)), dma((2, chunks, 2)), dma((2, chunks)), dma((2, chunks)),
            dma((chunks,)), dma((chunks,)),
        ],
        compiler_params=pltpu.CompilerParams(
            collective_id=0, has_side_effects=True, vmem_limit_bytes=64 * 1024 * 1000
        ),
    )(
        tokens, first_gain, u_proj, v_proj, group_gain, spatial, spatial_bias, mix_proj,
        second_gain, up_proj, down_proj,
    )


def layer_part(axes, *args):
    tokens, group_gain, spatial = args[0], args[4], args[5]
    fits = (
        axes["grp"] == 2
        and axes["fs"] == 4
        and axes["tp"] == 4
        and group_gain.shape[0] == 2
        and group_gain.shape[1] % 128 == 0
        and tokens.shape[0] % 256 == 0
        and tokens.shape[1] % 256 == 0
        and tokens.shape[1] == args[10].shape[1]
        and 256 % spatial.shape[1] == 0
    )
    return fused(*args) if fits else per_device(*args)


def solution(mesh):
    return jax.shard_map(
        functools.partial(layer_part, dict(mesh.shape)),
        mesh=mesh,
        in_specs=(
            P(("grp", "fs"), "tp"),
            P(),
            P("fs", "tp"),
            P("fs", "tp"),
            P("tp", None),
            P("tp", None, None),
            P("tp", None),
            P("fs", "tp"),
            P(),
            P("fs", "tp"),
            P("tp", "fs"),
        ),
        out_specs=P(("grp", "fs"), "tp"),
        check_vma=False,
    )
```

```python
import functools

import jax
import jax.numpy as jnp
from jax import lax
from jax.experimental import pallas as pl
from jax.experimental.pallas import tpu as pltpu
from jax.sharding import PartitionSpec as P

EPS = 1e-06


def rms_scale(values, gain_vec):
    mean_sq = jnp.mean(values * values, axis=-1, keepdims=True)
    return values * lax.rsqrt(mean_sq + EPS) * gain_vec.astype(jnp.float32)


def per_device(
    tokens,
    first_gain,
    u_proj,
    v_proj,
    group_gain,
    spatial,
    spatial_bias,
    mix_proj,
    second_gain,
    up_proj,
    down_proj,
):
    whole_rows = lax.all_gather(tokens, "tp", axis=1, tiled=True)
    row_count = whole_rows.shape[0]
    normed_rows = rms_scale(whole_rows.astype(jnp.float32), first_gain).astype(jnp.bfloat16)
    local_width = u_proj.shape[1]
    column_part = normed_rows
    u_pre = jnp.dot(
        column_part,
        lax.all_gather(u_proj, "fs", axis=0, tiled=True),
        preferred_element_type=jnp.float32,
    )
    v_pre = jnp.dot(
        column_part,
        lax.all_gather(v_proj, "fs", axis=0, tiled=True),
        preferred_element_type=jnp.float32,
    )
    u_act = jax.nn.gelu(u_pre).astype(jnp.bfloat16)
    local_groups = group_gain.shape[0]
    group_width = group_gain.shape[1]
    v_groups = jax.nn.gelu(v_pre).reshape(row_count, local_groups, group_width)
    v_normed = rms_scale(v_groups, group_gain).astype(jnp.bfloat16)
    block_len = spatial.shape[1]
    block_view = v_normed.reshape(row_count // block_len, block_len, local_groups, group_width)
    causal_mask = jnp.tril(jnp.ones((block_len, block_len), jnp.bool_))
    masked_weights = jnp.where(causal_mask[None], spatial, jnp.zeros_like(spatial))
    mixed_vals = jnp.einsum(
        "gts,nsgd->ntgd", masked_weights, block_view, preferred_element_type=jnp.float32
    )
    mixed_vals = mixed_vals + spatial_bias.astype(jnp.float32).T[None, :, :, None]
    gated_vals = (u_act.astype(jnp.float32) * mixed_vals.reshape(row_count, local_width)).astype(
        jnp.bfloat16
    )
    gated_whole = lax.all_gather(gated_vals, "tp", axis=1, tiled=True)
    column_part = gated_whole
    mix_vals = jnp.dot(
        column_part,
        lax.all_gather(mix_proj, "fs", axis=0, tiled=True),
        preferred_element_type=jnp.float32,
    )
    mid_stream = (tokens.astype(jnp.float32) + mix_vals).astype(jnp.bfloat16)
    mid_whole = lax.all_gather(mid_stream, "tp", axis=1, tiled=True)
    normed_two = rms_scale(mid_whole.astype(jnp.float32), second_gain).astype(jnp.bfloat16)
    column_part = normed_two
    pre_act = jnp.dot(
        column_part,
        lax.all_gather(up_proj, "fs", axis=0, tiled=True),
        preferred_element_type=jnp.float32,
    )
    hidden_act = jnp.square(jax.nn.relu(pre_act)).astype(jnp.bfloat16)
    down_terms = jnp.dot(
        hidden_act,
        lax.all_gather(down_proj, "fs", axis=1, tiled=True),
        preferred_element_type=jnp.float32,
    )
    down_sum = lax.psum_scatter(
        down_terms.astype(jnp.bfloat16), "tp", scatter_dimension=1, tiled=True
    ).astype(jnp.float32)
    return (mid_stream.astype(jnp.float32) + down_sum).astype(jnp.bfloat16)


def remote(src, dst, send, recv, where):
    return pltpu.make_async_remote_copy(
        src_ref=src,
        dst_ref=dst,
        send_sem=send,
        recv_sem=recv,
        device_id=where,
        device_id_type=pl.DeviceIdType.MESH,
    )


def fused_kernel(
    row_step,
    tok, gain1, u_w, v_w, ggain, spat, bias, mix_w, gain2, up_w, down_w,
    out,
    xg, uvg, mg, upg, dng, norm, gat, mid, hid, c_out, c_in, z_out, z_in, x_out, x_in,
    z_send, z_recv, y_send, y_recv, l_sem, a_send, a_recv, c_send, c_recv, r_send, r_recv,
    s_send, s_recv,
):
    y, z, t = lax.axis_index("grp"), lax.axis_index("fs"), lax.axis_index("tp")
    q, c, x = lax.rem(z, 2), lax.rem(t, 2), t // 2
    z_pair = z + 1 - 2 * q
    t_core, t_chip = t + 1 - 2 * c, lax.rem(t + 2, 4)
    to_y, to_z = (1 - y, z, t), (y, z_pair, t)
    to_c, to_x = (y, z, t_core), (y, z, t_chip)
    across, facing, pair = others = (lax.rem(z + 2, 4), 3 - z, z_pair)
    rows, width = tok.shape
    step = row_step
    f32, bf16 = jnp.float32, jnp.bfloat16

    barrier = pltpu.get_barrier_semaphore()
    for where in (to_y, to_c, to_x) + tuple((y, o, t) for o in others):
        pl.semaphore_signal(
            barrier, inc=1, device_id=where, device_id_type=pl.DeviceIdType.MESH
        )
    pl.semaphore_wait(barrier, 6)

    gw, da = ggain.shape[1], u_w.shape[1]
    ur, mr, pr, dr = u_w.shape[0], mix_w.shape[0], up_w.shape[0], down_w.shape[0] // 2

    def half(size, which):
        return pl.ds(pl.multiple_of(which * size, size), size)

    parts = (1, 1, 1, 2, 2)

    def take(w, par, which, k=0):
        shard = (u_w, v_w, mix_w, up_w, down_w)[w]
        if w == 4:
            if which is None:
                return shard.at[half(dr, par), :]
            return shard.at[half(dr // 4, 4 * par + 2 * which + k), :]
        tall = shard.shape[0]
        cols = slice(None) if w < 3 else half(shard.shape[1] // 2, par)
        if which is None:
            return shard.at[:, cols]
        return shard.at[half(tall // 2 // parts[w], parts[w] * which + k), cols]

    def put(w, source, which, k=0):
        n = parts[w]
        if w == 4:
            if which is None:
                return dng.at[source]
            return dng.at[source, half(dr // 2 // n, n * which + k), :]
        whole, tall = ((uvg, ur), (uvg, ur), (mg, mr), (upg, pr))[w]
        cols = pl.ds(w * da, da) if w < 2 else slice(None)
        if which is None:
            return whole.at[half(tall, source), cols]
        return whole.at[half(tall // 2 // n, n * (2 * source + which) + k), cols]

    def z_piece(w, dest, k):
        return remote(
            take(w, lax.rem(dest, 2), y, k), put(w, z, y, k), z_send.at[w, dest, k],
            z_recv.at[w, z, k], (y, dest, t),
        )

    def z_send_all(w, dest):
        for k in range(parts[w]):
            z_piece(w, dest, k).start()

    def y_piece(w, source, k):
        ref = put(w, source, y, k)
        return remote(ref, ref, y_send.at[w, source, k], y_recv.at[w, source, k], to_y)

    def y_arrived(w, source):
        for k in range(parts[w]):
            ref = put(w, source, 1 - y, k)
            remote(
                ref, ref, y_send.at[w, source, k], y_recv.at[w, source, k], to_y
            ).wait_recv()

    def forward(w, source):
        for k in range(parts[w]):
            ref = put(w, source, y, k)
            remote(
                ref, ref, z_send.at[w, source, k], z_recv.at[w, source, k], (y, source, t)
            ).wait_recv()
            y_piece(w, source, k).start()

    def pass_on(w):
        ref = put(w, across, y)
        remote(
            ref, ref, z_send.at[w, facing, 0], z_recv.at[w, across, 0], (y, pair, t)
        ).start()

    def own_copy(w):
        return pltpu.make_async_copy(take(w, q, None), put(w, z, None), l_sem.at[w])

    def gather_copy(a, h, n):
        p, s, where = (
            (q, t, to_z), (q, t, to_x), (q, t, to_c), (1 - q, t, to_x), (1 - q, t, to_c),
            (q, t_chip, to_c), (1 - q, t_chip, to_c),
        )[n]
        ref = piece(a, h, p, s)
        return remote(ref, ref, a_send.at[a, h, n], a_recv.at[a, h, n], where)

    def gather_arrived(a, h, n):
        p, s, where = (
            (1 - q, t, to_z), (q, t_chip, to_x), (q, t_core, to_c), (1 - q, t_chip, to_x),
            (1 - q, t_core, to_c), (q, 3 - t, to_c), (1 - q, 3 - t, to_c),
        )[n]
        ref = piece(a, h, p, s)
        return remote(ref, ref, a_send.at[a, h, n], a_recv.at[a, h, n], where)

    def piece(a, h, p, s):
        if a == 0:
            return xg.at[s, pl.ds(h * step, step), :]
        return gat.at[s, h] if a == 1 else mid.at[p, s, h]

    def gather_start(a, h):
        for n in (1, 2, 0)[: 3 if a == 2 else 2]:
            gather_copy(a, h, n).start()

    def gather_pair(a, h):
        gather_arrived(a, h, 0).wait_recv()
        gather_copy(a, h, 3).start()
        gather_copy(a, h, 4).start()

    def gather_rest(a, h):
        gather_arrived(a, h, 1).wait_recv()
        gather_copy(a, h, 5).start()
        if a == 2:
            gather_arrived(a, h, 3).wait_recv()
            gather_copy(a, h, 6).start()
        for n in (2, 4, 5, 6) if a == 2 else (2, 5):
            gather_arrived(a, h, n).wait_recv()

    chunks = rows // step
    inner = (z + 1) // 2 == 1

    own_tok = pltpu.make_async_copy(tok, xg.at[t], l_sem.at[5])
    own_tok.start()
    for o in (across, pair):
        for w in range(2):
            z_send_all(w, o)
    own_tok.wait()
    for h in range(chunks):
        gather_start(0, h)
    for w in range(5):
        own_copy(w).start()

    @pl.when(inner)
    def _():
        z_send_all(3, facing)

    for w in range(2):
        forward(w, across)
        pass_on(w)
    z_send_all(2, across)
    z_send_all(2, pair)
    for w in range(2):
        forward(w, pair)

    def scaled(pieces, gain):
        total = pieces[0].shape[0]
        sums = jnp.zeros((total, 1), f32)
        for piece in pieces:
            sums += jnp.sum(piece * piece, axis=-1, keepdims=True)
        count = sum(piece.shape[1] for piece in pieces)
        scale = lax.rsqrt(sums / count + EPS)
        at = 0
        res = []
        for piece in pieces:
            wide = piece.shape[1]
            res.append((piece * scale * gain[:, at : at + wide]).astype(bf16))
            at += wide
        return jnp.concatenate(res, axis=1)

    small = 64
    per_part = step // small
    gain_one = gain1[...].astype(f32).reshape(1, -1)
    gain_two = gain2[...].astype(f32).reshape(1, -1)

    def norm_one(h):
        def loop(i, carry):
            here = pl.ds(pl.multiple_of(h * step + i * small, small), small)
            norm[here, :] = scaled([xg[s, here, :].astype(f32) for s in range(4)], gain_one)
            return carry

        lax.fori_loop(0, per_part, loop, 0)

    blk = spat.shape[1]
    lower = lax.broadcasted_iota(jnp.int32, (blk, blk), 0) >= lax.broadcasted_iota(
        jnp.int32, (blk, blk), 1
    )
    eye = lax.broadcasted_iota(jnp.int32, (blk, blk), 0) == lax.broadcasted_iota(
        jnp.int32, (blk, blk), 1
    )
    mixers, shifts, gains = [], [], []
    for g in range(da // gw):
        mixers.append(jnp.where(lower, spat[g].astype(f32), 0.0).astype(bf16))
        column = jnp.where(eye, bias[g : g + 1, :].astype(f32), 0.0)
        shifts.append(jnp.sum(column, axis=1, keepdims=True))
        gains.append(ggain[g : g + 1, :].astype(f32))

    def mix_rows(h):
        both = jnp.dot(norm[pl.ds(h * step, step), :], uvg[...], preferred_element_type=f32)
        both = jax.nn.gelu(both)
        u_act = both[:, :da].astype(bf16).astype(f32)
        for g in range(da // gw):
            cols = slice(g * gw, (g + 1) * gw)
            v_act = both[:, da + g * gw : da + (g + 1) * gw]
            v_n = (
                v_act
                * lax.rsqrt(jnp.mean(v_act * v_act, axis=-1, keepdims=True) + EPS)
                * gains[g]
            ).astype(bf16)
            for b in range(step // blk):
                part = slice(b * blk, (b + 1) * blk)
                mixed = jnp.dot(mixers[g], v_n[part], preferred_element_type=f32) + shifts[g]
                gat[t, h, part, cols] = (u_act[part, cols] * mixed).astype(bf16)

    def middle_rows(h):
        left = jnp.concatenate([gat[k, h] for k in range(4)], axis=1)
        value = jnp.dot(left, mg[...], preferred_element_type=f32)
        value += tok[pl.ds(h * step, step), :].astype(f32)
        mid[q, t, h] = value.astype(bf16)

    def norm_two(h):
        def loop(i, carry):
            p, r = i // per_part, pl.multiple_of(lax.rem(i, per_part) * small, small)
            pieces = [mid[p, k, h, pl.ds(r, small), :].astype(f32) for k in range(4)]
            at = pl.multiple_of(h * 2 * step + i * small, small)
            norm[pl.ds(at, small), :] = scaled(pieces, gain_two)
            return carry

        lax.fori_loop(0, 2 * per_part, loop, 0)

    def up_rows(h):
        def loop(i, carry):
            here = pl.ds(pl.multiple_of((2 * h + i) * step, step), step)
            pre = jnp.dot(norm[here, :], upg[...], preferred_element_type=f32)
            hid[here, :] = jnp.square(jax.nn.relu(pre)).astype(bf16)
            return carry

        lax.fori_loop(0, 2, loop, 0)

    for h in range(chunks):
        gather_rest(0, h)
        norm_one(h)
    forward(2, across)
    pass_on(2)
    z_send_all(3, across)
    for w in range(2):
        forward(w, facing)
    for w in range(2):
        own_copy(w).wait()
        for o in others:
            y_arrived(w, o)
    for h in range(chunks):
        mix_rows(h)
        gather_start(1, h)
    forward(2, pair)
    forward(2, facing)

    @pl.when(inner)
    def _():
        z_send_all(4, facing)
        forward(3, facing)

    own_copy(2).wait()
    for h in range(chunks):
        gather_rest(1, h)
        if h == 0:
            for o in others:
                y_arrived(2, o)
        middle_rows(h)
        gather_start(2, h)
    forward(3, across)
    for h in range(chunks):
        gather_pair(2, h)

    @pl.when(jnp.logical_not(inner))
    def _():
        z_send_all(3, facing)

    z_send_all(3, pair)
    z_send_all(4, across)
    z_send_all(4, pair)

    @pl.when(jnp.logical_not(inner))
    def _():
        z_send_all(4, facing)

    for h in range(chunks):
        gather_rest(2, h)
        norm_two(h)

    @pl.when(inner)
    def _():
        forward(4, facing)

    @pl.when(jnp.logical_not(inner))
    def _():
        forward(3, facing)

    forward(3, pair)
    forward(4, across)
    own_copy(3).wait()
    for o in others:
        y_arrived(3, o)
    for h in range(chunks):
        up_rows(h)

    near, far = z // 2, 1 - z // 2
    order = (2 * near + 1 - c, 2 * near + c, 2 * far + 1 - c, 2 * far + c)

    def ready(quarter):
        @pl.when(quarter == z)
        def _():
            own_copy(4).wait()

        @pl.when(quarter != z)
        def _():
            y_arrived(4, quarter)

    def down_part(quarter, h, p):
        start = pl.multiple_of((2 * h + p) * step, step)
        return jnp.dot(
            hid[pl.ds(start, step), :], dng[quarter], preferred_element_type=f32
        )

    def core_copy(n, h, p):
        return remote(
            c_out.at[n, h, p], c_in.at[n, h, p], c_send.at[n, h, p], c_recv.at[n, h, p], to_c
        )

    def pair_copy(n, h):
        return remote(z_out.at[n, h], z_in.at[n, h], r_send.at[n, h], r_recv.at[n, h], to_z)

    def chip_copy(h):
        return remote(x_out.at[h], x_in.at[h], s_send.at[h], s_recv.at[h], to_x)

    def give(n):
        quarter = order[2 * n]
        ready(quarter)
        for i in range(2 * chunks):
            h, p = i % chunks, (1 - q if i < chunks else q)
            c_out[n, h, p] = down_part(quarter, h, p).astype(bf16)
            core_copy(n, h, p).start()

    def keep(n):
        quarter = order[2 * n + 1]
        ready(quarter)
        for i in range(2 * chunks):
            h, p = i % chunks, (1 - q if i < chunks else q)
            core_copy(n, h, p).wait_recv()
            value = down_part(quarter, h, p) + c_in[n, h, p].astype(f32)
            if i < chunks:
                z_out[n, h] = value.astype(bf16)
                pair_copy(n, h).start()
            else:
                c_in[n, h, p] = value.astype(bf16)

    forward(4, pair)
    give(0)

    @pl.when(jnp.logical_not(inner))
    def _():
        forward(4, facing)

    keep(0)
    give(1)
    keep(1)

    far_slot = jnp.where(near == x, 1, 0)
    own_slot = 1 - far_slot

    def send_far(n):
        for h in range(chunks):
            pair_copy(n, h).wait_recv()
            value = c_in[n, h, q].astype(f32) + z_in[n, h].astype(f32)
            x_out[h] = value.astype(bf16)
            chip_copy(h).start()

    @pl.when(far_slot == 0)
    def _():
        send_far(0)
        for h in range(chunks):
            pair_copy(1, h).wait_recv()

    @pl.when(far_slot == 1)
    def _():
        for h in range(chunks):
            pair_copy(0, h).wait_recv()
        send_far(1)

    for h in range(chunks):
        chip_copy(h).wait_recv()
        value = c_in[own_slot, h, q].astype(f32) + z_in[own_slot, h].astype(f32)
        value += x_in[h].astype(f32)
        out[pl.ds(h * step, step), :] = (value + mid[q, t, h].astype(f32)).astype(bf16)

    for w in range(5):
        for o in others:
            for k in range(parts[w]):
                z_piece(w, o, k).wait_send()
                y_piece(w, o, k).wait_send()
    for h in range(chunks):
        for a in range(3):
            for n in range(7) if a == 2 else (1, 2, 5):
                gather_copy(a, h, n).wait_send()
        for n in range(2):
            for p in range(2):
                core_copy(n, h, p).wait_send()
            pair_copy(n, h).wait_send()
        chip_copy(h).wait_send()


def fused(tokens, first_gain, u_proj, v_proj, group_gain, spatial, spatial_bias, mix_proj,
          second_gain, up_proj, down_proj):
    rows, width = tokens.shape
    both, wide, da = 2 * rows, second_gain.shape[0], u_proj.shape[1]
    vmem, bf16, dma = pltpu.VMEM, jnp.bfloat16, pltpu.SemaphoreType.DMA
    spec = pl.BlockSpec(memory_space=pltpu.VMEM)
    ff = up_proj.shape[1] // 2
    step = 256
    chunks = rows // step
    return pl.pallas_call(
        functools.partial(fused_kernel, step),
        out_shape=jax.ShapeDtypeStruct(tokens.shape, tokens.dtype),
        in_specs=[spec] * 11,
        out_specs=spec,
        scratch_shapes=[
            vmem((4, rows, width), bf16),
            vmem((wide, 2 * da), bf16),
            vmem((4 * mix_proj.shape[0], width), bf16),
            vmem((wide, ff), bf16),
            vmem((4, ff, down_proj.shape[1]), bf16),
            vmem((both, wide), bf16),
            vmem((4, chunks, step, da), bf16),
            vmem((2, 4, chunks, step, width), bf16),
            vmem((both, ff), bf16),
            vmem((2, chunks, 2, step, width), bf16),
            vmem((2, chunks, 2, step, width), bf16),
            vmem((2, chunks, step, width), bf16),
            vmem((2, chunks, step, width), bf16),
            vmem((chunks, step, width), bf16),
            vmem((chunks, step, width), bf16),
            dma((5, 4, 2)), dma((5, 4, 2)), dma((5, 4, 2)), dma((5, 4, 2)), dma((6,)),
            dma((3, chunks, 7)), dma((3, chunks, 7)),
            dma((2, chunks, 2)), dma((2, chunks, 2)), dma((2, chunks)), dma((2, chunks)),
            dma((chunks,)), dma((chunks,)),
        ],
        compiler_params=pltpu.CompilerParams(
            collective_id=0, has_side_effects=True, vmem_limit_bytes=64 * 1024 * 1000
        ),
    )(
        tokens, first_gain, u_proj, v_proj, group_gain, spatial, spatial_bias, mix_proj,
        second_gain, up_proj, down_proj,
    )


def layer_part(axes, *args):
    tokens, group_gain, spatial = args[0], args[4], args[5]
    fits = (
        axes["grp"] == 2
        and axes["fs"] == 4
        and axes["tp"] == 4
        and group_gain.shape[0] == 2
        and group_gain.shape[1] % 128 == 0
        and tokens.shape[0] % 256 == 0
        and tokens.shape[1] % 256 == 0
        and tokens.shape[1] == args[10].shape[1]
        and 256 % spatial.shape[1] == 0
    )
    return fused(*args) if fits else per_device(*args)


def solution(mesh):
    return jax.shard_map(
        functools.partial(layer_part, dict(mesh.shape)),
        mesh=mesh,
        in_specs=(
            P(("grp", "fs"), "tp"),
            P(),
            P("fs", "tp"),
            P("fs", "tp"),
            P("tp", None),
            P("tp", None, None),
            P("tp", None),
            P("fs", "tp"),
            P(),
            P("fs", "tp"),
            P("tp", "fs"),
        ),
        out_specs=P(("grp", "fs"), "tp"),
        check_vma=False,
    )
```
